32 devices in a mesh: ep: 8 (over z, x), tp: 4 (over y, core).
Axes of the slice: x: 2, y: 2, z: 4, core: 2. Of those that a mesh axis runs over, the one named last changes fastest.
Arguments:
- mix_bgate: bfloat16 [2048, 1024], P('ep', 'tp'), may hold values from -6 to 6
- mix_cgate: bfloat16 [2048, 1024], P('ep', 'tp'), may hold values from -6 to 6
- mix_input: bfloat16 [2048, 1024], P('ep', 'tp'), may hold values from -6 to 6
- conv_taps: float32 [3, 1024], P(None, 'tp'), may hold values from -3.5 to 3.5
- mix_out_w: bfloat16 [1024, 2048], P('tp'), may hold values from -0.1875 to 0.1875
- moe_x: bfloat16 [2048, 2048], P('ep', 'tp'), may hold values from -6 to 6
- moe_gain: float32 [2048], replicated, may hold values from 0.1 to 1.9
- routes: int32 [2048, 2], P('ep'), may hold values from 0 to 7, all different within a row; in each aligned block of 256 rows (0 to 255, 256 to 511, ...) at most 96 rows name the same one
- route_w: float32 [2048, 2], P('ep'), may hold values from 0.2 to 1
- w_gate: bfloat16 [8, 2048, 3584], P('ep', None, 'tp'), may hold values from -0.125 to 0.125
- w_up: bfloat16 [8, 2048, 3584], P('ep', None, 'tp'), may hold values from -0.125 to 0.125
- w_down: bfloat16 [8, 3584, 2048], P('ep', 'tp'), may hold values from -0.09375 to 0.09375
Outputs:
- mixed: bfloat16 [2048, 2048], P(('ep', 'tp'))
- routed: bfloat16 [2048, 2048], P('ep', 'tp')
The draws below stay inside these ranges and needn't reach their ends.
Inputs may be any that keep to these rules, and one draw needn't show every extreme that they name: `routes`: among the 256 rows of one index of ep, each row names 2 different experts and no expert is named by more than 96 rows; in every draw some expert is named by exactly 96 rows of some index.
All inputs are finite; a program needn't handle non-finite values.
Results may differ from the reference program's by a relative error of at most 0.012.
Values may be sent and summed in bfloat16 or wider, within the bound.
A program may use at most 64 MiB of HBM per device.

```python
import math
import jax
import jax.numpy as jnp
import numpy as np
from jax import lax

D = 2048
CONV = 1024
TAPS = 3
FF_E = 3584
TOPK = 2
TOK_MOE = 256
SEQ = 2048
MOE_TOKENS = 2048
EXPERTS = 8
CAP = 96
N_EP = 8
N_TP = 4


def steps_of(stream_key, shape, split, low, top_value):
    def one(position, shards_of):
        steps = jax.random.uniform(jax.random.fold_in(jax.random.fold_in(stream_key, 6), position), (shards_of,), jnp.float32, low / len(split), top_value / len(split))
        return jnp.repeat(jnp.exp(steps), shape[position] // shards_of).reshape((-1,) + (1,) * (len(shape) - position - 1))

    loudness = one(*split[0])
    for cut in split[1:]:
        loudness = loudness * one(*cut)
    return loudness


def assign_block(own_key, own, number, rows, amount, top, bound, skew):
    sequence = jax.random.permutation(own_key, amount)
    heavy_load, ordinary = portions_of(amount, rows * top, bound, skew, True), portions_of(amount, rows * top, bound, skew, False)
    places = jnp.arange(amount)

    def named(lengths, offset_by):
        used = int((lengths > 0).sum())
        fixed = max(1, used // 4)
        moved = fixed + (places - fixed + offset_by * (used - fixed)) % max(1, amount - fixed)
        return jnp.zeros((amount,), jnp.int32).at[sequence[jnp.where(places < fixed, places, moved)]].set(jnp.asarray(lengths, jnp.int32))

    lengths = jnp.where(number % 4 == 0, named(heavy_load, number // 4), named(ordinary, number - number // 4 - 1))
    mixed = jax.random.permutation(jax.random.fold_in(own, 3), amount)
    source_of, taker = mixed[0:amount // 2 * 2:2], mixed[1:amount // 2 * 2:2]
    slack = jnp.minimum(lengths[source_of] - 1, bound - lengths[taker]) // 2
    slack = jnp.where((source_of == sequence[0]) | (taker == sequence[0]) | (lengths[taker] == 0), 0, jnp.maximum(slack, 0))
    moved = jax.random.randint(jax.random.fold_in(own, 4), (amount // 2,), 0, 1 << 20) % (slack + 1)
    lengths = lengths.at[source_of].add(-moved).at[taker].add(moved)
    items = jnp.searchsorted(jnp.cumsum(lengths), jnp.arange(rows * top), side="right").astype(jnp.int32)
    listing = items.reshape(top, rows).T
    listing = listing[jax.random.permutation(jax.random.fold_in(own, 1), rows)]
    offset_by = jax.random.randint(jax.random.fold_in(own, 2), (rows, 1), 0, top)
    return jnp.take_along_axis(listing, (jnp.arange(top)[None, :] + offset_by) % top, axis=1)


def portions_of(amount, total, reach, lean, full):
    loads = [(1 << 20) // math.isqrt(grade ** lean) + 1 for grade in range(1, amount + 1)]
    largest = reach if full else min(reach, max(-(-total // amount), total * loads[0] // sum(loads)))
    least = 1 if total - largest >= amount - 1 else 0
    counts, surplus = [largest] + [least] * (amount - 1), total - largest - least * (amount - 1)
    while surplus > 0:
        candidates = [i for i in range(1, amount) if counts[i] < largest] or [i for i in range(1, amount) if counts[i] < reach]
        pool, budget = sum([loads[i] for i in candidates]), surplus
        for i in candidates:
            more = min(reach - counts[i], max(1, budget * loads[i] // pool), surplus)
            counts[i] = counts[i] + more
            surplus = surplus - more
    return np.array(counts)


def normal_values(rng, extent, spread, reach, shards=(), kind=jnp.bfloat16):
    factor_of = steps_of(rng, extent, shards, -0.22, 0.18) if shards else 1.0
    array = jax.random.normal(rng, extent, jnp.float32) * spread * factor_of
    return jnp.minimum(jnp.maximum(array, -reach), reach).astype(kind)


def setup_inputs(seed: int = 0) -> dict:
    key_of = jax.random.split(jax.random.key(seed), 13)
    mix_bgate = normal_values(key_of[0], (SEQ, CONV), 1.0, 6.0, ((0, 8), (1, 4)))
    mix_cgate = normal_values(key_of[1], (SEQ, CONV), 1.0, 6.0, ((0, 8), (1, 4)))
    mix_input = normal_values(key_of[2], (SEQ, CONV), 1.0, 6.0, ((0, 8), (1, 4)))
    conv_taps = normal_values(key_of[3], (TAPS, CONV), TAPS ** -0.5, 3.5, ((1, 4),), jnp.float32)
    mix_out_w = normal_values(key_of[4], (CONV, D), CONV ** -0.5, 0.1875, ((0, 4),))
    moe_x = normal_values(key_of[5], (MOE_TOKENS, D), 1.0, 6.0, ((0, 8), (1, 4)))
    moe_gain = jnp.clip(1.0 + 0.18 * jax.random.normal(key_of[6], (D,), jnp.float32), 0.1, 1.9)
    routes_keys = jax.random.split(jax.random.fold_in(key_of[7], 1), MOE_TOKENS // TOK_MOE)
    routes_turns = jax.random.permutation(jax.random.fold_in(key_of[7], 3), MOE_TOKENS // TOK_MOE)
    routes = jax.vmap(lambda own, number: assign_block(jax.random.fold_in(key_of[7], 2), own, number, TOK_MOE, EXPERTS, TOPK, CAP, 2))(routes_keys, routes_turns).reshape((MOE_TOKENS, TOPK))
    route_w = jnp.clip(0.2 + 0.8 * jax.random.uniform(key_of[8], (MOE_TOKENS, TOPK), jnp.float32) ** steps_of(key_of[8], (MOE_TOKENS, TOPK), ((0, 8),), -0.2, 0.2), 0.2, 1.0)
    w_gate = normal_values(key_of[9], (EXPERTS, D, FF_E), D ** -0.5, 0.125, ((0, 8), (2, 4)))
    w_up = normal_values(key_of[10], (EXPERTS, D, FF_E), D ** -0.5, 0.125, ((0, 8), (2, 4)))
    w_down = normal_values(key_of[11], (EXPERTS, FF_E, D), FF_E ** -0.5, 0.09375, ((0, 8), (1, 4)))
    return {"mix_bgate": mix_bgate, "mix_cgate": mix_cgate, "mix_input": mix_input, "conv_taps": conv_taps, "mix_out_w": mix_out_w, "moe_x": moe_x, "moe_gain": moe_gain, "routes": routes, "route_w": route_w, "w_gate": w_gate, "w_up": w_up, "w_down": w_down}


def rms_rows(values, gain):
    wide = values.astype(jnp.float32)
    scale = lax.rsqrt(lax.optimization_barrier(jnp.mean(wide * wide, axis=-1, keepdims=True)) + 1e-06)
    return (wide * scale * gain).astype(jnp.bfloat16)

def rounded(value):
    return lax.optimization_barrier(value.astype(jnp.bfloat16)).astype(jnp.float32)

def reference(mix_bgate, mix_cgate, mix_input, conv_taps, mix_out_w, moe_x, moe_gain, routes, route_w, w_gate, w_up, w_down):
    length = mix_input.shape[0]
    prod = mix_cgate.astype(jnp.float32) * mix_input.astype(jnp.float32)
    padded = jnp.pad(prod, ((TAPS - 1, 0), (0, 0)))
    conv = conv_taps[0] * padded[0:length]
    for j in range(1, TAPS):
        conv = conv + conv_taps[j] * padded[j:j + length]
    gated = (mix_bgate.astype(jnp.float32) * conv).astype(jnp.bfloat16)
    step = CONV // N_TP
    total = jnp.zeros((length, D), jnp.float32)
    for q in range(N_TP):
        part = jnp.dot(gated[:, q * step:(q + 1) * step], mix_out_w[q * step:(q + 1) * step], preferred_element_type=jnp.float32)
        total = total + rounded(part)
    mixed = total.astype(jnp.bfloat16)
    normed = rms_rows(moe_x, moe_gain)
    dev_routes = routes.reshape(N_EP, TOK_MOE * TOPK)
    onehot = (dev_routes[:, :, None] == jnp.arange(EXPERTS, dtype=jnp.int32)[None, None, :]).astype(jnp.int32)
    earlier = jnp.cumsum(onehot, axis=1) - onehot
    slot = lax.optimization_barrier(jnp.sum(earlier * onehot, axis=2))
    row = jnp.arange(N_EP, dtype=jnp.int32)[:, None] * CAP + slot
    flat_e = dev_routes.reshape(-1)
    flat_row = row.reshape(-1).astype(jnp.int32)
    token = jnp.arange(MOE_TOKENS * TOPK, dtype=jnp.int32) // TOPK
    buffers = jnp.zeros((EXPERTS, N_EP * CAP, D), jnp.bfloat16).at[flat_e, flat_row].set(normed[token])
    fstep = FF_E // N_TP

    def expert(items):
        rows, wg, wu, wd = items
        gate = jnp.dot(rows, wg, preferred_element_type=jnp.float32)
        upper = jnp.dot(rows, wu, preferred_element_type=jnp.float32)
        hidden = (jax.nn.silu(gate) * upper).astype(jnp.bfloat16)
        acc = jnp.zeros((rows.shape[0], D), jnp.float32)
        for q in range(N_TP):
            part = jnp.dot(hidden[:, q * fstep:(q + 1) * fstep], wd[q * fstep:(q + 1) * fstep], preferred_element_type=jnp.float32)
            acc = acc + rounded(part)
        return acc.astype(jnp.bfloat16)
    results = lax.map(expert, (buffers, w_gate, w_up, w_down))
    picked = results[flat_e, flat_row].astype(jnp.float32).reshape(MOE_TOKENS, TOPK, D)
    routed = lax.optimization_barrier(jnp.sum(picked * route_w[:, :, None], axis=1)).astype(jnp.bfloat16)
    return (mixed, routed)
```

```python
import jax
import jax.numpy as jnp
from jax import lax
from jax.sharding import PartitionSpec as P


CHUNKS = 2


def shifted(block, axis, distance):
    devices = range(lax.axis_size(axis))
    route = [(i - distance, i) for i in devices if i - distance in devices]
    return lax.ppermute(block, axis, route)


def conv_mixer(mix_bgate, mix_cgate, mix_input, conv_taps, mix_out_w):
    length = mix_input.shape[0]
    reach = conv_taps.shape[0] - 1
    tail = jnp.stack([mix_cgate[length - reach :], mix_input[length - reach :]])
    before = shifted(tail, "ep", 1)
    gates_c = jnp.concatenate([before[0], mix_cgate], 0).astype(jnp.float32)
    inputs_h = jnp.concatenate([before[1], mix_input], 0).astype(jnp.float32)
    prod = gates_c * inputs_h
    conv = conv_taps[0] * prod[0:length]
    for j in range(1, reach + 1):
        conv = conv + conv_taps[j] * prod[j : j + length]
    gated = (mix_bgate.astype(jnp.float32) * conv).astype(jnp.bfloat16)
    return jnp.dot(gated, mix_out_w, preferred_element_type=jnp.float32).astype(jnp.bfloat16)


def chunk_edges(cap, count):
    base = cap // count
    return [(i * base, cap if i == count - 1 else (i + 1) * base) for i in range(count)]


def route_tables(routes, experts, cap):
    ntok, top = routes.shape
    chosen = routes[:, :, None] == jnp.arange(experts, dtype=jnp.int32)
    named = jnp.any(chosen, axis=1)
    row = lax.broadcasted_iota(jnp.int32, (ntok, ntok), 0)
    col = lax.broadcasted_iota(jnp.int32, (ntok, ntok), 1)
    rank = jnp.dot(
        (col < row).astype(jnp.bfloat16),
        named.astype(jnp.bfloat16),
        preferred_element_type=jnp.float32,
    ).astype(jnp.int32)
    return chosen, named, rank


def norm_rows(parts, gain):
    n_tp, rows, d = parts.shape
    wide = parts.astype(jnp.float32)
    total = jnp.sum(wide * wide, axis=(0, 2))
    scale = lax.rsqrt(total / (n_tp * d) + 1e-06)[:, None]
    pieces = [
        (wide[i] * scale * gain[i * d : (i + 1) * d]).astype(jnp.bfloat16) for i in range(n_tp)
    ]
    return jnp.concatenate(pieces, axis=1)


def experts_part(parts, moe_gain, w_gate, w_up, w_down):
    n_tp, n_ep, per_dev, c, d = parts.shape
    normed = norm_rows(parts.reshape(n_tp, n_ep * per_dev * c, d), moe_gain)
    normed = normed.reshape(n_ep, per_dev, c, n_tp * d)
    outs = []
    for e in range(per_dev):
        rows = normed[:, e].reshape(n_ep * c, n_tp * d)
        gate = jnp.dot(rows, w_gate[e], preferred_element_type=jnp.float32)
        upper = jnp.dot(rows, w_up[e], preferred_element_type=jnp.float32)
        hidden = (jax.nn.silu(gate) * upper).astype(jnp.bfloat16)
        down = jnp.dot(hidden, w_down[e], preferred_element_type=jnp.float32)
        outs.append(down.astype(jnp.bfloat16).reshape(n_ep, c, -1))
    return jnp.stack(outs, axis=1)


def body(
    mix_bgate,
    mix_cgate,
    mix_input,
    conv_taps,
    mix_out_w,
    moe_x,
    moe_gain,
    routes,
    route_w,
    w_gate,
    w_up,
    w_down,
):
    ntok, d = moe_x.shape
    top = routes.shape[1]
    n_ep = lax.axis_size("ep")
    n_tp = lax.axis_size("tp")
    per_dev = w_gate.shape[0]
    experts = per_dev * n_ep
    cap = 4 * ((3 * ntok * top + 8 * experts - 1) // (8 * experts))
    edges = chunk_edges(cap, CHUNKS)

    share = conv_mixer(mix_bgate, mix_cgate, mix_input, conv_taps, mix_out_w)
    share, moe_x = lax.optimization_barrier((share, moe_x))
    mixed = lax.psum_scatter(share, "tp", scatter_dimension=0, tiled=True)

    chosen, named, rank = route_tables(routes, experts, cap)
    landed = []
    for lo, hi in edges:
        slots = jnp.arange(lo, hi, dtype=jnp.int32)
        pick = named.T[:, None, :] & (rank.T[:, None, :] == slots[None, :, None])
        pick = pick.astype(jnp.bfloat16).reshape(experts * (hi - lo), ntok)
        out = jnp.dot(pick, moe_x, preferred_element_type=jnp.float32).astype(jnp.bfloat16)
        out = out.reshape(n_ep, per_dev, hi - lo, d)
        landed.append(lax.all_to_all(out, "ep", split_axis=0, concat_axis=0, tiled=True))
    gathered = [lax.all_gather(x, "tp", axis=0, tiled=False) for x in landed]
    returned = []
    down = None
    for parts in gathered:
        if down is not None:
            parts, down = lax.optimization_barrier((parts, down))
        down = experts_part(parts, moe_gain, w_gate, w_up, w_down)
        summed = lax.psum_scatter(down, "tp", scatter_dimension=3, tiled=True)
        returned.append(lax.all_to_all(summed, "ep", split_axis=0, concat_axis=0, tiled=True))
    total = jnp.zeros((top * ntok, d), jnp.float32)
    for (lo, hi), back in zip(edges, returned):
        slots = jnp.arange(lo, hi, dtype=jnp.int32)
        at = jnp.moveaxis(chosen, 1, 0)[:, :, :, None] & (rank[:, :, None] == slots)[None]
        at = at.astype(jnp.bfloat16).reshape(top * ntok, experts * (hi - lo))
        total = total + jnp.dot(
            at, back.reshape(experts * (hi - lo), d), preferred_element_type=jnp.float32
        )
    picked = total.reshape(top, ntok, d)
    routed = jnp.sum(picked * route_w.T[:, :, None], axis=0).astype(jnp.bfloat16)
    return (mixed, routed)


def solution(mesh):
    in_specs = (
        P("ep", "tp"),
        P("ep", "tp"),
        P("ep", "tp"),
        P(None, "tp"),
        P("tp", None),
        P("ep", "tp"),
        P(),
        P("ep", None),
        P("ep", None),
        P("ep", None, "tp"),
        P("ep", None, "tp"),
        P("ep", "tp", None),
    )
    out_specs = (P(("ep", "tp"), None), P("ep", "tp"))
    return jax.shard_map(body, mesh=mesh, in_specs=in_specs, out_specs=out_specs, check_vma=False)
```

```python
import jax
import jax.numpy as jnp
from jax import lax
from jax.sharding import PartitionSpec as P


CHUNKS = 2


def shifted(block, axis, distance):
    devices = range(lax.axis_size(axis))
    route = [(i - distance, i) for i in devices if i - distance in devices]
    return lax.ppermute(block, axis, route)


def conv_mixer(mix_bgate, mix_cgate, mix_input, conv_taps, mix_out_w):
    length = mix_input.shape[0]
    reach = conv_taps.shape[0] - 1
    tail = jnp.stack([mix_cgate[length - reach :], mix_input[length - reach :]])
    before = shifted(tail, "ep", 1)
    gates_c = jnp.concatenate([before[0], mix_cgate], 0).astype(jnp.float32)
    inputs_h = jnp.concatenate([before[1], mix_input], 0).astype(jnp.float32)
    prod = gates_c * inputs_h
    conv = conv_taps[0] * prod[0:length]
    for j in range(1, reach + 1):
        conv = conv + conv_taps[j] * prod[j : j + length]
    gated = (mix_bgate.astype(jnp.float32) * conv).astype(jnp.bfloat16)
    return jnp.dot(gated, mix_out_w, preferred_element_type=jnp.float32).astype(jnp.bfloat16)


def swapped(block, axis, bit):
    return lax.ppermute(block, axis, [(i, i ^ bit) for i in range(lax.axis_size(axis))])


def axis_bits(axis):
    size = lax.axis_size(axis)
    assert size & (size - 1) == 0
    return [1 << b for b in range(size.bit_length() - 1)]


def gather_parts(block, axis):
    bits = axis_bits(axis)
    held = {0: block}
    for bit in reversed(bits):
        for j in sorted(held, reverse=True):
            held[j ^ bit] = swapped(held[j], axis, bit)
    me = lax.axis_index(axis)
    for bit in bits:
        away = (me & bit) != 0
        held = {i: jnp.where(away, held[i ^ bit], held[i]) for i in held}
    return [held[i] for i in range(len(held))]


def scatter_sum(block, axis, dim):
    size = lax.axis_size(axis)
    width = block.shape[dim] // size
    me = lax.axis_index(axis)
    held = {
        j: lax.dynamic_slice_in_dim(block, (me ^ j) * width, width, dim) for j in range(size)
    }
    for bit in axis_bits(axis):
        for j in sorted((j for j in held if j & bit), reverse=True):
            arrived = swapped(held.pop(j), axis, bit).astype(jnp.float32)
            total = held[j ^ bit].astype(jnp.float32) + arrived
            held[j ^ bit] = total if j == bit else total.astype(jnp.bfloat16)
    return held[0].astype(jnp.bfloat16)


def chunk_edges(cap, count):
    base = cap // count
    return [(i * base, cap if i == count - 1 else (i + 1) * base) for i in range(count)]


def route_tables(routes, experts, cap):
    ntok, top = routes.shape
    chosen = routes[:, :, None] == jnp.arange(experts, dtype=jnp.int32)
    named = jnp.any(chosen, axis=1)
    row = lax.broadcasted_iota(jnp.int32, (ntok, ntok), 0)
    col = lax.broadcasted_iota(jnp.int32, (ntok, ntok), 1)
    rank = jnp.dot(
        (col < row).astype(jnp.bfloat16),
        named.astype(jnp.bfloat16),
        preferred_element_type=jnp.float32,
    ).astype(jnp.int32)
    return chosen, named, rank


def norm_rows(parts, gain):
    n_tp, d = len(parts), parts[0].shape[1]
    wide = [part.astype(jnp.float32) for part in parts]
    total = sum(jnp.sum(piece * piece, axis=1) for piece in wide)
    scale = lax.rsqrt(total / (n_tp * d) + 1e-06)[:, None]
    pieces = [
        (wide[i] * scale * gain[i * d : (i + 1) * d]).astype(jnp.bfloat16) for i in range(n_tp)
    ]
    return jnp.concatenate(pieces, axis=1)


def experts_part(parts, moe_gain, w_gate, w_up, w_down):
    n_tp = len(parts)
    n_ep, per_dev, c, d = parts[0].shape
    normed = norm_rows([part.reshape(n_ep * per_dev * c, d) for part in parts], moe_gain)
    normed = normed.reshape(n_ep, per_dev, c, n_tp * d)
    outs = []
    for e in range(per_dev):
        rows = normed[:, e].reshape(n_ep * c, n_tp * d)
        gate = jnp.dot(rows, w_gate[e], preferred_element_type=jnp.float32)
        upper = jnp.dot(rows, w_up[e], preferred_element_type=jnp.float32)
        hidden = (jax.nn.silu(gate) * upper).astype(jnp.bfloat16)
        down = jnp.dot(hidden, w_down[e], preferred_element_type=jnp.float32)
        outs.append(down.astype(jnp.bfloat16).reshape(n_ep, c, -1))
    return jnp.stack(outs, axis=1)


def body(
    mix_bgate,
    mix_cgate,
    mix_input,
    conv_taps,
    mix_out_w,
    moe_x,
    moe_gain,
    routes,
    route_w,
    w_gate,
    w_up,
    w_down,
):
    ntok, d = moe_x.shape
    top = routes.shape[1]
    n_ep = lax.axis_size("ep")
    n_tp = lax.axis_size("tp")
    per_dev = w_gate.shape[0]
    experts = per_dev * n_ep
    cap = 4 * ((3 * ntok * top + 8 * experts - 1) // (8 * experts))
    edges = chunk_edges(cap, CHUNKS)

    share = conv_mixer(mix_bgate, mix_cgate, mix_input, conv_taps, mix_out_w)
    share, moe_x = lax.optimization_barrier((share, moe_x))
    mixed = scatter_sum(share, "tp", 0)

    chosen, named, rank = route_tables(routes, experts, cap)
    landed = []
    for lo, hi in edges:
        slots = jnp.arange(lo, hi, dtype=jnp.int32)
        pick = named.T[:, None, :] & (rank.T[:, None, :] == slots[None, :, None])
        pick = pick.astype(jnp.bfloat16).reshape(experts * (hi - lo), ntok)
        out = jnp.dot(pick, moe_x, preferred_element_type=jnp.float32).astype(jnp.bfloat16)
        out = out.reshape(n_ep, per_dev, hi - lo, d)
        landed.append(lax.all_to_all(out, "ep", split_axis=0, concat_axis=0, tiled=True))
    gathered = [gather_parts(x, "tp") for x in landed]
    returned = []
    down = None
    for parts in gathered:
        if down is not None:
            moe_gain = moe_gain + 0.0 * down[0, 0, 0, 0].astype(jnp.float32)
        down = experts_part(parts, moe_gain, w_gate, w_up, w_down)
        summed = scatter_sum(down, "tp", 3)
        returned.append(lax.all_to_all(summed, "ep", split_axis=0, concat_axis=0, tiled=True))
    total = jnp.zeros((top * ntok, d), jnp.float32)
    for (lo, hi), back in zip(edges, returned):
        slots = jnp.arange(lo, hi, dtype=jnp.int32)
        at = jnp.moveaxis(chosen, 1, 0)[:, :, :, None] & (rank[:, :, None] == slots)[None]
        at = at.astype(jnp.bfloat16).reshape(top * ntok, experts * (hi - lo))
        total = total + jnp.dot(
            at, back.reshape(experts * (hi - lo), d), preferred_element_type=jnp.float32
        )
    picked = total.reshape(top, ntok, d)
    routed = jnp.sum(picked * route_w.T[:, :, None], axis=0).astype(jnp.bfloat16)
    return (mixed, routed)


def solution(mesh):
    in_specs = (
        P("ep", "tp"),
        P("ep", "tp"),
        P("ep", "tp"),
        P(None, "tp"),
        P("tp", None),
        P("ep", "tp"),
        P(),
        P("ep", None),
        P("ep", None),
        P("ep", None, "tp"),
        P("ep", None, "tp"),
        P("ep", "tp", None),
    )
    out_specs = (P(("ep", "tp"), None), P("ep", "tp"))
    return jax.shard_map(body, mesh=mesh, in_specs=in_specs, out_specs=out_specs, check_vma=False)
```
